32 devices in a mesh: gr: 2 (over x), fs: 8 (over z, y), tp: 2 (over core).
Axes of the slice: x: 2, y: 2, z: 4, core: 2. Of those that a mesh axis runs over, the one named last changes fastest.
Arguments:
- tokens: bfloat16 [16384, 3072], P(('gr', 'fs')), may hold values from -6 to 6
- norm_gain: float32 [3072], P(('gr', 'fs')), may hold values from 0.1 to 1.9
- gate_weight: float32 [8, 3072, 768], P(None, ('gr', 'fs'), 'tp'), may hold values from -0.109375 to 0.109375
- up_weight: float32 [8, 3072, 768], P(None, ('gr', 'fs'), 'tp'), may hold values from -0.109375 to 0.109375
- down_weight: float32 [8, 3072, 768], P(None, ('gr', 'fs'), 'tp'), may hold values from -0.21875 to 0.21875
- group_pick: int32 [16384], P(('gr', 'fs')), may hold values from 0 to 3, as said below
- expert_pick: int32 [16384, 2], P(('gr', 'fs')), may hold values from 0 to 1, as said below
- route_weight: float32 [16384, 2], P(('gr', 'fs')), may hold values from 0.1 to 1
Outputs:
- combined: bfloat16 [16384, 3072], P(('gr', 'fs'), 'tp')
- gate_served: bfloat16 [8, 3072, 768], P('fs', None, 'tp')
- up_served: bfloat16 [8, 3072, 768], P('fs', None, 'tp')
- down_served: bfloat16 [8, 3072, 768], P('fs', None, 'tp')
The draws below stay inside these ranges and needn't reach their ends.
Inputs may be any that keep to these rules, and one draw needn't show every extreme that they name: `group_pick`: in each aligned block of 1024 rows every group is picked by the same number of rows. `expert_pick`: the 2 entries of a row differ. In each aligned block of 1024 rows, every expert (group and number together) is named exactly 256 times.
All inputs are finite; a program needn't handle non-finite values.
Results may differ from the reference program's by a relative error of at most 0.0092.
Values may be sent and summed in bfloat16 or wider, within the bound.
A program may use at most 128 MiB of HBM per device.

```python
import math
import jax
import jax.numpy as jnp
from jax import lax

D = 3072
FF = 768
GROUPS = 4
TOP = 2
TOK_DEV = 1024
EXPERTS = 8
TOKENS = 16384
N_TP = 2


def routing(key):
    blocks = TOKENS // TOK_DEV
    per_group = EXPERTS // GROUPS
    position = jnp.arange(TOK_DEV, dtype=jnp.int32)
    group_of = position % GROUPS
    within = position // GROUPS
    first_pick = within % per_group
    second_pick = (first_pick + 1 + within // per_group % (per_group - 1)) % per_group

    def one_block(block_key):
        order_key, label_key = jax.random.split(block_key)
        order = jax.random.permutation(order_key, TOK_DEV)
        relabel = jax.vmap(lambda label_one: jax.random.permutation(label_one, per_group))(jax.random.split(label_key, GROUPS))
        first_label = relabel[group_of, first_pick]
        second_label = relabel[group_of, second_pick]
        pairs = jnp.stack([first_label, second_label], axis=1).astype(jnp.int32)
        group_tok = jnp.zeros((TOK_DEV,), jnp.int32).at[order].set(group_of)
        pair_tok = jnp.zeros((TOK_DEV, 2), jnp.int32).at[order].set(pairs)
        return (group_tok, pair_tok)
    block_keys = jax.random.split(jax.random.fold_in(key, 71), blocks)
    groups_all, pairs_all = jax.vmap(one_block)(block_keys)
    return (groups_all.reshape(TOKENS).astype(jnp.int32), pairs_all.reshape(TOKENS, 2).astype(jnp.int32))


def draw_group_pick(key, part):
    return routing(key)[0]


def draw_expert_pick(key, part):
    return routing(key)[1]


def block_levels(own_key, dims, pieces, low, high):
    def one(dim, shards_of):
        heights = jax.random.uniform(jax.random.fold_in(jax.random.fold_in(own_key, 6), dim), (shards_of,), jnp.float32, low / len(pieces), high / len(pieces))
        return jnp.repeat(jnp.exp(heights), dims[dim] // shards_of).reshape((-1,) + (1,) * (len(dims) - dim - 1))

    loudness = one(*pieces[0])
    for cut in pieces[1:]:
        loudness = loudness * one(*cut)
    return loudness


def centred(own_key, extent, spread, bound, pieces=(), held_as=jnp.bfloat16):
    result = jax.random.normal(own_key, extent, jnp.float32) * spread
    if len(pieces) > 0:
        result = block_levels(own_key, extent, pieces, -0.22, 0.18) * result
    return jnp.clip(result, min=-bound, max=bound).astype(held_as)


def setup_inputs(seed: int = 0) -> dict:
    key_of = jax.random.split(jax.random.key(seed), 9)
    return {
        "tokens": centred(key_of[0], (TOKENS, D), 1.0, 6.0, ((0, 16),)),
        "norm_gain": jnp.clip(1.0 + 0.18 * jax.random.normal(key_of[1], (D,), jnp.float32), 0.1, 1.9),
        "gate_weight": centred(key_of[2], (EXPERTS, D, FF), D ** -0.5, 0.109375, ((1, 16), (2, 2)), jnp.float32),
        "up_weight": centred(key_of[3], (EXPERTS, D, FF), D ** -0.5, 0.109375, ((1, 16), (2, 2)), jnp.float32),
        "down_weight": centred(key_of[4], (EXPERTS, D, FF), FF ** -0.5, 0.21875, ((1, 16), (2, 2)), jnp.float32),
        "group_pick": draw_group_pick(jax.random.fold_in(key_of[8], 71), 0),
        "expert_pick": draw_expert_pick(jax.random.fold_in(key_of[8], 71), 0),
        "route_weight": jnp.clip(jnp.exp(math.log(1.0) - 2.3025851 * jax.random.uniform(key_of[7], (TOKENS, TOP), jnp.float32) ** block_levels(key_of[7], (TOKENS, TOP), ((0, 16),), -0.2, 0.2)), 0.1, 1.0),
    }


EPS = 1e-06

def reference(tokens, norm_gain, gate_weight, up_weight, down_weight, group_pick, expert_pick, route_weight):
    gate_served = (norm_gain[None, :, None] * gate_weight).astype(jnp.bfloat16)
    up_served = (norm_gain[None, :, None] * up_weight).astype(jnp.bfloat16)
    down_served = down_weight.astype(jnp.bfloat16)
    as_float = tokens.astype(jnp.float32)
    normed = (as_float * lax.rsqrt(lax.optimization_barrier(jnp.mean(as_float * as_float, axis=-1, keepdims=True)) + EPS)).astype(jnp.bfloat16)
    expert_ids = (group_pick[:, None] * (EXPERTS // GROUPS) + expert_pick).reshape(-1).astype(jnp.int32)
    per_expert = TOP * TOKENS // EXPERTS
    half_width = FF // N_TP

    def run_expert(expert_item):
        w_gate, w_up, w_down, index = expert_item
        row_ids = jnp.nonzero(expert_ids == index, size=per_expert)[0]
        rows_in = normed[row_ids // TOP]
        gate_acts = jnp.dot(rows_in, w_gate, preferred_element_type=jnp.float32)
        up_acts = jnp.dot(rows_in, w_up, preferred_element_type=jnp.float32)
        hidden = (jax.nn.silu(gate_acts) * up_acts).astype(jnp.bfloat16)
        accum_sum = jnp.zeros((per_expert, D), jnp.float32)
        for block in range(N_TP):
            part_sum = lax.dot_general(hidden[:, block * half_width:(block + 1) * half_width], w_down[:, block * half_width:(block + 1) * half_width], (((1,), (1,)), ((), ())), preferred_element_type=jnp.float32)
            accum_sum = accum_sum + lax.optimization_barrier(part_sum.astype(jnp.bfloat16)).astype(jnp.float32)
        return (accum_sum.astype(jnp.bfloat16), row_ids)
    outputs, row_ids = lax.map(run_expert, (gate_served, up_served, down_served, jnp.arange(EXPERTS, dtype=jnp.int32)))
    flat_out = jnp.zeros((TOP * TOKENS, D), jnp.bfloat16).at[row_ids.reshape(-1)].set(outputs.reshape(-1, D))
    combined = lax.optimization_barrier(jnp.sum(route_weight[:, :, None] * flat_out.reshape(TOKENS, TOP, D).astype(jnp.float32), axis=1))
    return (combined.astype(jnp.bfloat16), gate_served, up_served, down_served)
```

```python
import jax
import jax.numpy as jnp
from jax import lax
from jax.sharding import PartitionSpec as P

GROUPS = 4


EPS = 1e-06


def local_spread(
    tokens, norm_gain, gate_weight, up_weight, down_weight, group_pick, expert_pick, route_weight
):
    scaled = norm_gain[None, :, None]
    gate_local = (scaled * gate_weight).astype(jnp.bfloat16)
    up_local = (scaled * up_weight).astype(jnp.bfloat16)
    down_local = down_weight.astype(jnp.bfloat16)
    experts, rows_dev, cols_dev = gate_local.shape
    gate_four = gate_local.reshape(experts, 1, rows_dev, cols_dev)
    up_four = up_local.reshape(experts, 1, rows_dev, cols_dev)
    down_four = down_local.reshape(experts, 1, rows_dev, cols_dev)
    gathered = (
        lax.all_gather(gate_four, "gr", axis=1, tiled=True),
        lax.all_gather(up_four, "gr", axis=1, tiled=True),
        lax.all_gather(down_four, "gr", axis=1, tiled=True),
    )
    relaid = (
        lax.all_to_all(gathered[0], "fs", split_axis=0, concat_axis=2, tiled=True),
        lax.all_to_all(gathered[1], "fs", split_axis=0, concat_axis=2, tiled=True),
        lax.all_to_all(gathered[2], "fs", split_axis=0, concat_axis=2, tiled=True),
    )
    gate_new = relaid[0].reshape(1, -1, cols_dev)
    up_new = relaid[1].reshape(1, -1, cols_dev)
    down_new = relaid[2].reshape(1, -1, cols_dev)
    tok_rows, model_width = tokens.shape
    as_float = tokens.astype(jnp.float32)
    normed = (
        as_float * lax.rsqrt(jnp.mean(as_float * as_float, axis=-1, keepdims=True) + EPS)
    ).astype(jnp.bfloat16)
    per_group = experts // GROUPS
    top_count = expert_pick.shape[1]
    capacity = top_count * tok_rows // experts
    flat_ids = (group_pick[:, None] * per_group + expert_pick).reshape(-1)
    onehot = (flat_ids[:, None] == jnp.arange(experts, dtype=jnp.int32)[None, :]).astype(jnp.int32)
    slot_index = jnp.sum(onehot * (jnp.cumsum(onehot, axis=0) - 1), axis=1)
    target = flat_ids * capacity + slot_index
    source = (
        jnp.zeros((experts * capacity,), jnp.int32)
        .at[target]
        .set(jnp.arange(top_count * tok_rows, dtype=jnp.int32) // top_count)
    )
    outgoing = normed[source].reshape(experts, capacity, model_width)
    share = capacity // lax.axis_size("tp")
    start = lax.axis_index("tp") * share
    my_share = lax.dynamic_slice_in_dim(outgoing, start, share, 1)
    landed = lax.all_to_all(my_share, "fs", split_axis=0, concat_axis=1, tiled=True).reshape(
        experts, share, model_width
    )
    arrived = lax.all_gather(landed, "tp", axis=1, tiled=True).reshape(-1, model_width)
    gate_acts = jnp.dot(arrived, gate_new[0], preferred_element_type=jnp.float32)
    up_acts = jnp.dot(arrived, up_new[0], preferred_element_type=jnp.float32)
    hidden = (jax.nn.silu(gate_acts) * up_acts).astype(jnp.bfloat16)
    partial_value = lax.dot_general(
        hidden, down_new[0], (((1,), (1,)), ((), ())), preferred_element_type=jnp.float32
    ).astype(jnp.bfloat16)
    summed = (
        lax.psum_scatter(partial_value, "tp", scatter_dimension=1, tiled=True)
        .astype(jnp.float32)
        .astype(jnp.bfloat16)
    )
    returned = lax.all_to_all(summed, "fs", split_axis=0, concat_axis=0, tiled=True)
    picked = returned[target].reshape(tok_rows, top_count, -1).astype(jnp.float32)
    combined = jnp.sum(route_weight[:, :, None] * picked, axis=1).astype(jnp.bfloat16)
    return (combined, gate_new, up_new, down_new)


def local_whole_group(
    tokens, norm_gain, gate_weight, up_weight, down_weight, group_pick, expert_pick, route_weight
):
    experts, rows_dev, cols_dev = gate_weight.shape
    tok_rows, model_width = tokens.shape
    per_group = experts // GROUPS
    n_tp = lax.axis_size("tp")
    share = tok_rows // GROUPS // n_tp
    own = share * GROUPS
    columns = [[g * per_group + j for g in range(GROUPS)] for j in range(per_group)]
    members = [[g * per_group + j for j in range(per_group)] for g in range(GROUPS)]

    scaled = norm_gain[None, :, None]
    served = []
    for value in (scaled * gate_weight, scaled * up_weight, down_weight):
        moved = lax.all_to_all(
            value.astype(jnp.bfloat16), "fs", split_axis=0, concat_axis=1, tiled=True
        )
        served.append(lax.all_gather(moved, "gr", axis=1, tiled=True))
    gate_new, up_new, down_new = served

    onehot = (group_pick[None, :] == jnp.arange(GROUPS, dtype=jnp.int32)[:, None]).astype(
        jnp.bfloat16
    )
    row = lax.broadcasted_iota(jnp.int32, (tok_rows, tok_rows), 0)
    col = lax.broadcasted_iota(jnp.int32, (tok_rows, tok_rows), 1)
    before = jnp.dot(onehot, (row < col).astype(jnp.bfloat16), preferred_element_type=jnp.float32)
    rank = jnp.sum(onehot.astype(jnp.float32) * before, axis=0).astype(jnp.int32)
    place = rank // share * own + group_pick * share + rank % share

    as_float = tokens.astype(jnp.float32)
    normed = (
        as_float * lax.rsqrt(jnp.mean(as_float * as_float, axis=-1, keepdims=True) + EPS)
    ).astype(jnp.bfloat16)
    first = lax.axis_index("tp") * own
    slots = first + lax.broadcasted_iota(jnp.int32, (own, tok_rows), 0)
    select = (slots == place[None, :]).astype(jnp.bfloat16)
    outgoing = jnp.dot(select, normed, preferred_element_type=jnp.float32).astype(jnp.bfloat16)

    member = jnp.arange(per_group, dtype=jnp.int32)
    by_member = jnp.sum(
        jnp.where(expert_pick[:, :, None] == member, route_weight[:, :, None], 0.0), axis=1
    )
    weights_out = jnp.sum(
        jnp.where((row == place[None, :])[None], by_member.T[:, None, :], 0.0), axis=2
    )
    weights_out = weights_out.reshape(per_group, n_tp, GROUPS, share)
    weights_in = lax.all_to_all(
        weights_out, "fs", split_axis=2, concat_axis=2, axis_index_groups=columns, tiled=True
    )

    landed = lax.all_to_all(
        outgoing.reshape(GROUPS, share, model_width),
        "fs",
        split_axis=0,
        concat_axis=0,
        axis_index_groups=columns,
        tiled=True,
    )
    shared = lax.all_gather(landed, "fs", axis=0, axis_index_groups=members)
    arrived = lax.all_gather(shared, "tp", axis=0).reshape(-1, model_width)
    gate_acts = jnp.dot(arrived, gate_new[0], preferred_element_type=jnp.float32)
    up_acts = jnp.dot(arrived, up_new[0], preferred_element_type=jnp.float32)
    hidden = (jax.nn.silu(gate_acts) * up_acts).astype(jnp.bfloat16)
    partial_value = lax.dot_general(
        hidden, down_new[0], (((1,), (1,)), ((), ())), preferred_element_type=jnp.float32
    ).astype(jnp.bfloat16)
    summed = lax.psum_scatter(partial_value, "tp", scatter_dimension=1, tiled=True)
    width = summed.shape[1]
    paired = lax.all_to_all(
        summed.reshape(n_tp, per_group, GROUPS, share, width),
        "fs",
        split_axis=1,
        concat_axis=1,
        axis_index_groups=members,
        tiled=True,
    )
    mixed = sum(
        weights_in[j][..., None] * paired[:, j].astype(jnp.float32) for j in range(per_group)
    ).astype(jnp.bfloat16)
    returned = lax.all_to_all(
        mixed, "fs", split_axis=1, concat_axis=1, axis_index_groups=columns, tiled=True
    ).reshape(tok_rows, width)
    restore = (col == place[:, None]).astype(jnp.bfloat16)
    combined = jnp.dot(restore, returned, preferred_element_type=jnp.float32).astype(jnp.bfloat16)
    return (combined, gate_new, up_new, down_new)


def local(tokens, norm_gain, gate, up, down, group_pick, expert_pick, route_weight):
    whole_group = gate.shape[0] // GROUPS == expert_pick.shape[1]
    body = local_whole_group if whole_group else local_spread
    return body(tokens, norm_gain, gate, up, down, group_pick, expert_pick, route_weight)


def solution(mesh):
    in_specs = (
        P(("gr", "fs"), None),
        P(("gr", "fs")),
        P(None, ("gr", "fs"), "tp"),
        P(None, ("gr", "fs"), "tp"),
        P(None, ("gr", "fs"), "tp"),
        P(("gr", "fs")),
        P(("gr", "fs"), None),
        P(("gr", "fs"), None),
    )
    out_specs = (
        P(("gr", "fs"), "tp"),
        P("fs", None, "tp"),
        P("fs", None, "tp"),
        P("fs", None, "tp"),
    )
    return jax.shard_map(local, mesh=mesh, in_specs=in_specs, out_specs=out_specs, check_vma=False)
```

```python
import jax
import jax.numpy as jnp
from jax import lax
from jax.experimental import pallas as pl
from jax.experimental.pallas import tpu as pltpu
from jax.sharding import PartitionSpec as P

GROUPS = 4


EPS = 1e-06


def local_spread(
    tokens, norm_gain, gate_weight, up_weight, down_weight, group_pick, expert_pick, route_weight
):
    scaled = norm_gain[None, :, None]
    gate_local = (scaled * gate_weight).astype(jnp.bfloat16)
    up_local = (scaled * up_weight).astype(jnp.bfloat16)
    down_local = down_weight.astype(jnp.bfloat16)
    experts, rows_dev, cols_dev = gate_local.shape
    gate_four = gate_local.reshape(experts, 1, rows_dev, cols_dev)
    up_four = up_local.reshape(experts, 1, rows_dev, cols_dev)
    down_four = down_local.reshape(experts, 1, rows_dev, cols_dev)
    gathered = (
        lax.all_gather(gate_four, "gr", axis=1, tiled=True),
        lax.all_gather(up_four, "gr", axis=1, tiled=True),
        lax.all_gather(down_four, "gr", axis=1, tiled=True),
    )
    relaid = (
        lax.all_to_all(gathered[0], "fs", split_axis=0, concat_axis=2, tiled=True),
        lax.all_to_all(gathered[1], "fs", split_axis=0, concat_axis=2, tiled=True),
        lax.all_to_all(gathered[2], "fs", split_axis=0, concat_axis=2, tiled=True),
    )
    gate_new = relaid[0].reshape(1, -1, cols_dev)
    up_new = relaid[1].reshape(1, -1, cols_dev)
    down_new = relaid[2].reshape(1, -1, cols_dev)
    tok_rows, model_width = tokens.shape
    as_float = tokens.astype(jnp.float32)
    normed = (
        as_float * lax.rsqrt(jnp.mean(as_float * as_float, axis=-1, keepdims=True) + EPS)
    ).astype(jnp.bfloat16)
    per_group = experts // GROUPS
    top_count = expert_pick.shape[1]
    capacity = top_count * tok_rows // experts
    flat_ids = (group_pick[:, None] * per_group + expert_pick).reshape(-1)
    onehot = (flat_ids[:, None] == jnp.arange(experts, dtype=jnp.int32)[None, :]).astype(jnp.int32)
    slot_index = jnp.sum(onehot * (jnp.cumsum(onehot, axis=0) - 1), axis=1)
    target = flat_ids * capacity + slot_index
    source = (
        jnp.zeros((experts * capacity,), jnp.int32)
        .at[target]
        .set(jnp.arange(top_count * tok_rows, dtype=jnp.int32) // top_count)
    )
    outgoing = normed[source].reshape(experts, capacity, model_width)
    share = capacity // lax.axis_size("tp")
    start = lax.axis_index("tp") * share
    my_share = lax.dynamic_slice_in_dim(outgoing, start, share, 1)
    landed = lax.all_to_all(my_share, "fs", split_axis=0, concat_axis=1, tiled=True).reshape(
        experts, share, model_width
    )
    arrived = lax.all_gather(landed, "tp", axis=1, tiled=True).reshape(-1, model_width)
    gate_acts = jnp.dot(arrived, gate_new[0], preferred_element_type=jnp.float32)
    up_acts = jnp.dot(arrived, up_new[0], preferred_element_type=jnp.float32)
    hidden = (jax.nn.silu(gate_acts) * up_acts).astype(jnp.bfloat16)
    partial_value = lax.dot_general(
        hidden, down_new[0], (((1,), (1,)), ((), ())), preferred_element_type=jnp.float32
    ).astype(jnp.bfloat16)
    summed = (
        lax.psum_scatter(partial_value, "tp", scatter_dimension=1, tiled=True)
        .astype(jnp.float32)
        .astype(jnp.bfloat16)
    )
    returned = lax.all_to_all(summed, "fs", split_axis=0, concat_axis=0, tiled=True)
    picked = returned[target].reshape(tok_rows, top_count, -1).astype(jnp.float32)
    combined = jnp.sum(route_weight[:, :, None] * picked, axis=1).astype(jnp.bfloat16)
    return (combined, gate_new, up_new, down_new)


def greet(peers):
    barrier = pltpu.get_barrier_semaphore()
    for peer in peers:
        pl.semaphore_signal(barrier, inc=1, device_id=peer, device_id_type=pl.DeviceIdType.MESH)
    pl.semaphore_wait(barrier, len(peers))


def remote(src, dst, send, recv, peer):
    return pltpu.make_async_remote_copy(
        src_ref=src,
        dst_ref=dst,
        send_sem=send,
        recv_sem=recv,
        device_id=peer,
        device_id_type=pl.DeviceIdType.MESH,
    )


def dispatch(tokens_out, gate_out, up_out, down_out):
    groups, share, width = tokens_out.shape
    n_fs, rows, cols = gate_out.shape
    n_gr, n_tp = lax.axis_size("gr"), lax.axis_size("tp")
    members = n_fs // groups
    n_weights = 3

    def kernel(tok, w0, w1, w2, arrived, s0, s1, s2, sends, local, rz, ry, rt, rw, rg):
        fs, gr, tp = lax.axis_index("fs"), lax.axis_index("gr"), lax.axis_index("tp")
        g, j = fs // members, fs % members
        out_w, in_w = (w0, w1, w2), (s0, s1, s2)
        fs_peers = [{"fs": (fs + s) % n_fs} for s in range(1, n_fs)]
        gr_peers = [{"gr": (gr + s) % n_gr} for s in range(1, n_gr)]
        tp_peers = [{"tp": (tp + s) % n_tp} for s in range(1, n_tp)]
        greet(fs_peers + gr_peers + tp_peers)
        started = []

        def send(src, dst, recv, peer):
            copy = remote(src, dst, sends.at[len(started)], recv, peer)
            copy.start()
            started.append(copy)

        def landed(ref, recv):
            remote(ref, ref, sends.at[0], recv, tp_peers[0]).wait_recv()

        for s in range(1, groups):
            z = (g + s) % groups
            send(tok.at[z], arrived.at[tp, j, g], rz.at[g], {"fs": z * members + j})
        for s in range(1, n_fs):
            d = (fs + s) % n_fs
            for w in range(n_weights):
                send(out_w[w].at[d], in_w[w].at[gr, fs], rw.at[w, fs], {"fs": d})
        locals_ = [pltpu.make_async_copy(tok.at[g], arrived.at[tp, j, g], local.at[n_weights])]
        for w in range(n_weights):
            locals_.append(
                pltpu.make_async_copy(out_w[w].at[fs], in_w[w].at[gr, fs], local.at[w])
            )
        for copy in locals_:
            copy.start()

        for s in range(groups):
            z = (g + groups - s) % groups
            slot = arrived.at[tp, j, z]
            if s:
                landed(slot, rz.at[z])
            source = slot if s else tok.at[g]
            for m in range(1, members):
                send(source, slot, ry.at[j, z], {"fs": g * members + (j + m) % members})
            for peer in tp_peers:
                send(source, slot, rt.at[j, z], peer)
        for s in range(n_fs):
            d = (fs + n_fs - s) % n_fs
            for w in range(n_weights):
                slot = in_w[w].at[gr, d]
                if s:
                    landed(slot, rw.at[w, d])
                for peer in gr_peers:
                    send(slot if s else out_w[w].at[fs], slot, rg.at[w, d], peer)
        for m in range(1, members):
            other = (j + m) % members
            for s in range(groups):
                z = (g + groups - s) % groups
                slot = arrived.at[tp, other, z]
                landed(slot, ry.at[other, z])
                for peer in tp_peers:
                    send(slot, slot, rt.at[other, z], peer)
        for t in range(1, n_tp):
            for m in range(members):
                for z in range(groups):
                    landed(arrived.at[(tp + t) % n_tp, m, z], rt.at[m, z])
        for q in range(1, n_gr):
            for w in range(n_weights):
                for d in range(n_fs):
                    landed(in_w[w].at[(gr + q) % n_gr, d], rg.at[w, d])
        for copy in locals_:
            copy.wait()
        for copy in started:
            copy.wait_send()

    n_sends = (
        groups - 1
        + n_weights * (n_fs - 1)
        + groups * (members - 1 + n_tp - 1)
        + n_weights * n_fs * (n_gr - 1)
        + groups * (members - 1) * (n_tp - 1)
    )
    served = jax.ShapeDtypeStruct((n_gr, n_fs, rows, cols), jnp.bfloat16)
    dma = pltpu.SemaphoreType.DMA
    out = pl.pallas_call(
        kernel,
        out_shape=(
            jax.ShapeDtypeStruct((n_tp, members, groups, share, width), jnp.bfloat16),
            served,
            served,
            served,
        ),
        in_specs=[pl.BlockSpec(memory_space=pltpu.VMEM)] * 4,
        out_specs=[pl.BlockSpec(memory_space=pl.ANY)] * 4,
        scratch_shapes=[
            dma((n_sends,)),
            dma((n_weights + 1,)),
            dma((groups,)),
            dma((members, groups)),
            dma((members, groups)),
            dma((n_weights, n_fs)),
            dma((n_weights, n_fs)),
        ],
        compiler_params=pltpu.CompilerParams(
            collective_id=0, has_side_effects=True, vmem_limit_bytes=60 * 2**20
        ),
        name="dispatch",
    )(tokens_out, gate_out, up_out, down_out)
    return out[0], [x.reshape(1, -1, cols) for x in out[1:]]


def give_back(summed, weights_in):
    n_tp, members, groups, share, width = summed.shape

    def kernel(own, weight, home, others, mixed, send_y, recv_y, send_z, recv_z):
        fs = lax.axis_index("fs")
        g, j = fs // members, fs % members
        mates = [{"fs": g * members + (j + m) % members} for m in range(1, members)]
        greet(mates + [{"fs": (g + s) % groups * members + j} for s in range(1, groups)])
        order = [s % groups for s in range(1, groups + 1)]
        copies = []
        for s in order:
            z = (g + s) % groups
            for t in range(n_tp):
                for m in range(1, members):
                    copy = remote(
                        own.at[t, (j + m) % members, z],
                        others.at[members - m - 1, t, z],
                        send_y.at[m - 1, t, s],
                        recv_y.at[members - m - 1, t, z],
                        mates[m - 1],
                    )
                    copy.start()
                    copies.append(copy)
        for s in order:
            z = (g + s) % groups
            for t in range(n_tp):
                total = weight[j, t, z] * own[t, j, z].astype(jnp.float32)
                for m in range(1, members):
                    slot = others.at[m - 1, t, z]
                    remote(
                        slot, slot, send_y.at[0, 0, 0], recv_y.at[m - 1, t, z], mates[m - 1]
                    ).wait_recv()
                    total += weight[(j + m) % members, t, z] * others[m - 1, t, z].astype(
                        jnp.float32
                    )
                if s:
                    mixed[s - 1, t] = total.astype(jnp.bfloat16)
                    copy = remote(
                        mixed.at[s - 1, t],
                        home.at[t, g],
                        send_z.at[t, s - 1],
                        recv_z.at[t, g],
                        {"fs": z * members + j},
                    )
                    copy.start()
                    copies.append(copy)
                else:
                    home[t, g] = total.astype(jnp.bfloat16)
        for s in range(1, groups):
            z = (g + s) % groups
            for t in range(n_tp):
                slot = home.at[t, z]
                remote(
                    slot, slot, send_z.at[0, 0], recv_z.at[t, z], {"fs": z * members + j}
                ).wait_recv()
        for copy in copies:
            copy.wait_send()

    dma = pltpu.SemaphoreType.DMA
    return pl.pallas_call(
        kernel,
        out_shape=jax.ShapeDtypeStruct((n_tp, groups, share, width), jnp.bfloat16),
        in_specs=[pl.BlockSpec(memory_space=pltpu.VMEM)] * 2,
        out_specs=pl.BlockSpec(memory_space=pltpu.VMEM),
        scratch_shapes=[
            pltpu.VMEM((members - 1, n_tp, groups, share, width), jnp.bfloat16),
            pltpu.VMEM((groups - 1, n_tp, share, width), jnp.bfloat16),
            dma((members - 1, n_tp, groups)),
            dma((members - 1, n_tp, groups)),
            dma((n_tp, groups - 1)),
            dma((n_tp, groups)),
        ],
        compiler_params=pltpu.CompilerParams(
            collective_id=1, has_side_effects=True, vmem_limit_bytes=60 * 2**20
        ),
        name="give_back",
    )(summed, weights_in)


def local_whole_group(
    tokens, norm_gain, gate_weight, up_weight, down_weight, group_pick, expert_pick, route_weight
):
    experts, rows_dev, cols_dev = gate_weight.shape
    tok_rows, model_width = tokens.shape
    per_group = experts // GROUPS
    n_tp = lax.axis_size("tp")
    share = tok_rows // GROUPS // n_tp
    own = share * GROUPS
    columns = [[g * per_group + j for g in range(GROUPS)] for j in range(per_group)]

    scaled = norm_gain[None, :, None]
    to_serve = [
        value.astype(jnp.bfloat16) for value in (scaled * gate_weight, scaled * up_weight, down_weight)
    ]

    onehot = (group_pick[None, :] == jnp.arange(GROUPS, dtype=jnp.int32)[:, None]).astype(
        jnp.bfloat16
    )
    row = lax.broadcasted_iota(jnp.int32, (tok_rows, tok_rows), 0)
    col = lax.broadcasted_iota(jnp.int32, (tok_rows, tok_rows), 1)
    before = jnp.dot(onehot, (row < col).astype(jnp.bfloat16), preferred_element_type=jnp.float32)
    rank = jnp.sum(onehot.astype(jnp.float32) * before, axis=0).astype(jnp.int32)
    place = rank // share * own + group_pick * share + rank % share

    as_float = tokens.astype(jnp.float32)
    normed = (
        as_float * lax.rsqrt(jnp.mean(as_float * as_float, axis=-1, keepdims=True) + EPS)
    ).astype(jnp.bfloat16)
    first = lax.axis_index("tp") * own
    slots = first + lax.broadcasted_iota(jnp.int32, (own, tok_rows), 0)
    select = (slots == place[None, :]).astype(jnp.bfloat16)
    outgoing = jnp.dot(select, normed, preferred_element_type=jnp.float32).astype(jnp.bfloat16)

    member = jnp.arange(per_group, dtype=jnp.int32)
    by_member = jnp.sum(
        jnp.where(expert_pick[:, :, None] == member, route_weight[:, :, None], 0.0), axis=1
    )
    weights_out = jnp.sum(
        jnp.where((row == place[None, :])[None], by_member.T[:, None, :], 0.0), axis=2
    )
    weights_out = weights_out.reshape(per_group, n_tp, GROUPS, share)
    weights_in = lax.all_to_all(
        weights_out, "fs", split_axis=2, concat_axis=2, axis_index_groups=columns, tiled=True
    )

    arrived, (gate_new, up_new, down_new) = dispatch(
        outgoing.reshape(GROUPS, share, model_width), *to_serve
    )
    arrived = arrived.reshape(-1, model_width)
    gate_acts = jnp.dot(arrived, gate_new[0], preferred_element_type=jnp.float32)
    up_acts = jnp.dot(arrived, up_new[0], preferred_element_type=jnp.float32)
    hidden = (jax.nn.silu(gate_acts) * up_acts).astype(jnp.bfloat16)
    partial_value = lax.dot_general(
        hidden, down_new[0], (((1,), (1,)), ((), ())), preferred_element_type=jnp.float32
    ).astype(jnp.bfloat16)
    summed = lax.psum_scatter(partial_value, "tp", scatter_dimension=1, tiled=True)
    width = summed.shape[1]
    returned = give_back(
        summed.reshape(n_tp, per_group, GROUPS, share, width), weights_in[..., None]
    ).reshape(tok_rows, width)
    restore = (col == place[:, None]).astype(jnp.bfloat16)
    combined = jnp.dot(restore, returned, preferred_element_type=jnp.float32).astype(jnp.bfloat16)
    return (combined, gate_new, up_new, down_new)


def local(tokens, norm_gain, gate, up, down, group_pick, expert_pick, route_weight):
    whole_group = gate.shape[0] // GROUPS == expert_pick.shape[1]
    body = local_whole_group if whole_group else local_spread
    return body(tokens, norm_gain, gate, up, down, group_pick, expert_pick, route_weight)


def solution(mesh):
    in_specs = (
        P(("gr", "fs"), None),
        P(("gr", "fs")),
        P(None, ("gr", "fs"), "tp"),
        P(None, ("gr", "fs"), "tp"),
        P(None, ("gr", "fs"), "tp"),
        P(("gr", "fs")),
        P(("gr", "fs"), None),
        P(("gr", "fs"), None),
    )
    out_specs = (
        P(("gr", "fs"), "tp"),
        P("fs", None, "tp"),
        P("fs", None, "tp"),
        P("fs", None, "tp"),
    )
    return jax.shard_map(local, mesh=mesh, in_specs=in_specs, out_specs=out_specs, check_vma=False)
```
